32 devices in a mesh: dp: 4 (over y, x), kv: 4 (over z), tp: 2 (over core).
Axes of the slice: x: 2, y: 2, z: 4, core: 2. Of those that a mesh axis runs over, the one named last changes fastest.
Arguments:
- tokens: bfloat16 [32, 4, 2048], P('dp', None, 'kv'), may hold values from -600 to 600
- input_norm_gain: float32 [2048], P('kv'), may hold values from 0.1 to 1.9
- query_projection: bfloat16 [2048, 1024], P('kv', 'tp'), may hold values from -0.125 to 0.125
- key_projection: bfloat16 [2048, 1024], P('kv', 'tp'), may hold values from -0.125 to 0.125
- value_projection: bfloat16 [2048, 1024], P('kv', 'tp'), may hold values from -0.125 to 0.125
- write_strength_weight: bfloat16 [2048, 16], P('kv', 'tp'), may hold values from -0.125 to 0.125
- decay_projection: bfloat16 [2048, 16], P('kv', 'tp'), may hold values from -0.125 to 0.125
- head_decay_rate: float32 [16], P('tp'), may hold values from 0.02 to 0.6
- token_extra_decay: float32 [32, 4, 16], P(('dp', 'kv'), None, 'tp'), may hold values from -0.7 to 0
- accepted: int32 [32], P(('dp', 'kv')), may hold values from 1 to 4
- prior_step_states: float32 [32, 4, 16, 4096], P(('dp', 'kv'), None, 'tp'), may hold values from -4 to 4
- output_norm_gain: float32 [64], replicated, may hold values from 0.1 to 1.9
- output_projection: bfloat16 [1024, 2048], P('tp', 'kv'), may hold values from -0.1875 to 0.1875
Outputs:
- mixed: bfloat16 [32, 4, 2048], P('dp', None, 'kv')
- updated_states: float32 [32, 4, 16, 4096], P(('dp', 'kv'), None, 'tp')
The draws below stay inside these ranges and needn't reach their ends.
Inputs may be any that keep to these rules, and one draw needn't show every extreme that they name: `accepted`: how many proposals of the previous step each sequence kept; its state after that many is taken up.
All inputs are finite; a program needn't handle non-finite values.
Results may differ from the reference program's by a relative error of at most 0.029.
Values may be sent and summed in bfloat16 or wider, within the bound.
A program may use at most 64 MiB of HBM per device.

```python
import math
import jax
import jax.numpy as jnp
from jax import lax

D = 2048
HEAD_TOTAL = 16
HEAD = 64
DRAFT_TOKENS = 4
SEQ_DEV = 2
SEQUENCE_TOTAL = 32


def draw_tokens(key, part):
    base_key = jax.random.fold_in(key, 11)
    key_one = jax.random.fold_in(base_key, 0)
    column = jnp.arange(D, dtype=jnp.float32) / D
    sample_noise = jax.random.normal(key_one, (SEQUENCE_TOTAL, DRAFT_TOKENS, D), jnp.float32)
    values = sample_noise * 10.0 ** column
    return values.astype(jnp.bfloat16)


def place_ends(array, own_key, least, largest):
    place = [jax.random.randint(jax.random.fold_in(own_key, axis), (), 0, length) for axis, length in enumerate(array.shape)]
    longest = array.shape.index(max(array.shape))
    next_to = place[:longest] + [(place[longest] + 1) % array.shape[longest]] + place[longest + 1:]
    return array.at[tuple(place)].set(least).at[tuple(next_to)].set(largest)


def shard_levels(key, extent, pieces, smallest, largest):
    factor_of, own = 1.0, jax.random.fold_in(key, 6)
    for dim, parts in pieces:
        heights = jnp.exp(jax.random.uniform(jax.random.fold_in(own, dim), (parts,), jnp.float32, smallest / len(pieces), largest / len(pieces)))
        factor_of = factor_of * jnp.repeat(heights, extent[dim] // parts).reshape([-1 if axis == dim else 1 for axis in range(len(extent))])
    return factor_of


def scatter_about(own_key, extent, scale, bound, cuts=(), held_as=jnp.bfloat16):
    array = jax.random.normal(own_key, extent, jnp.float32) * scale
    if len(cuts) > 0:
        array = shard_levels(own_key, extent, cuts, -0.22, 0.18) * array
    return jnp.clip(array, min=-bound, max=bound).astype(held_as)


def setup_inputs(seed: int = 0) -> dict:
    key_list = jax.random.split(jax.random.key(seed), 14)
    tokens = draw_tokens(jax.random.fold_in(key_list[13], 71), 0)
    input_norm_gain = jnp.clip(1.0 + 0.18 * jax.random.normal(key_list[1], (D,), jnp.float32), 0.1, 1.9)
    query_projection = scatter_about(key_list[2], (D, HEAD_TOTAL * HEAD), D ** -0.5, 0.125, ((0, 4), (1, 2)))
    key_projection = scatter_about(key_list[3], (D, HEAD_TOTAL * HEAD), D ** -0.5, 0.125, ((0, 4), (1, 2)))
    value_projection = scatter_about(key_list[4], (D, HEAD_TOTAL * HEAD), D ** -0.5, 0.125, ((0, 4), (1, 2)))
    write_strength_weight = scatter_about(key_list[5], (D, HEAD_TOTAL), D ** -0.5, 0.125, ((0, 4), (1, 2)))
    decay_projection = scatter_about(key_list[6], (D, HEAD_TOTAL), D ** -0.5, 0.125, ((0, 4), (1, 2)))
    head_decay_rate = jnp.clip(jnp.exp(math.log(0.6) - 3.4011974 * jax.random.uniform(key_list[7], (HEAD_TOTAL,), jnp.float32) ** shard_levels(key_list[7], (HEAD_TOTAL,), ((0, 2),), -0.2, 0.2)), 0.02, 0.6)
    token_extra_decay = jnp.clip(-0.7 + 0.7 * jax.random.uniform(key_list[8], (SEQUENCE_TOTAL, DRAFT_TOKENS, HEAD_TOTAL), jnp.float32) ** shard_levels(key_list[8], (SEQUENCE_TOTAL, DRAFT_TOKENS, HEAD_TOTAL), ((0, 16), (2, 2)), -0.2, 0.2), -0.7, 0.0)
    accepted = place_ends(jax.random.randint(key_list[9], (SEQUENCE_TOTAL,), 1, DRAFT_TOKENS + 1), jax.random.fold_in(key_list[9], 1), 1, DRAFT_TOKENS).astype(jnp.int32)
    prior_step_states = scatter_about(key_list[10], (SEQUENCE_TOTAL, DRAFT_TOKENS, HEAD_TOTAL, HEAD * HEAD), 0.3, 4.0, ((0, 16), (2, 2)), jnp.float32)
    output_norm_gain = jnp.clip(1.0 + 0.18 * jax.random.normal(key_list[11], (HEAD,), jnp.float32), 0.1, 1.9)
    output_projection = scatter_about(key_list[12], (HEAD_TOTAL * HEAD, D), (HEAD_TOTAL * HEAD) ** -0.5, 0.1875, ((0, 2), (1, 4)))
    return {"tokens": tokens, "input_norm_gain": input_norm_gain, "query_projection": query_projection, "key_projection": key_projection, "value_projection": value_projection, "write_strength_weight": write_strength_weight, "decay_projection": decay_projection, "head_decay_rate": head_decay_rate, "token_extra_decay": token_extra_decay, "accepted": accepted, "prior_step_states": prior_step_states, "output_norm_gain": output_norm_gain, "output_projection": output_projection}


epsilon = 1e-06
highest = lax.Precision.HIGHEST

def unit_rows(values):
    return values * lax.rsqrt(lax.optimization_barrier(jnp.sum(values * values, axis=-1, keepdims=True)) + epsilon)

def delta_block(query_heads, key_heads, value_heads, beta_gate, decay_logarithm, start_state):
    proposal_len = query_heads.shape[2]
    cumulative = jnp.cumsum(decay_logarithm, axis=-1)
    spread = cumulative[..., :, None] - cumulative[..., None, :]
    strict = jnp.tril(jnp.ones((proposal_len, proposal_len), bool), -1)
    inclusive = jnp.tril(jnp.ones((proposal_len, proposal_len), bool))
    key_inner = jnp.einsum('nhid,nhjd->nhij', key_heads, key_heads, precision=highest)
    coupling = jnp.where(strict, beta_gate[..., :, None] * key_inner * jnp.exp(jnp.where(strict, spread, 0.0)), 0.0)
    growth = jnp.exp(cumulative)
    right_w = (beta_gate * growth)[..., None] * key_heads
    right_u = beta_gate[..., None] * value_heads
    solved_w = []
    solved_u = []
    for current in range(proposal_len):
        part_w = right_w[:, :, current]
        part_u = right_u[:, :, current]
        for earlier in range(current):
            factor = coupling[:, :, current, earlier][..., None]
            part_w = part_w - factor * solved_w[earlier]
            part_u = part_u - factor * solved_u[earlier]
        solved_w.append(part_w)
        solved_u.append(part_u)
    weights_w = jnp.stack(solved_w, axis=2)
    weights_u = jnp.stack(solved_u, axis=2)
    corrected = weights_u - jnp.einsum('nhpd,nhde->nhpe', weights_w, start_state, precision=highest)
    within = jnp.where(inclusive, jnp.exp(jnp.where(inclusive, spread, 0.0)), 0.0)
    scores = jnp.einsum('nhid,nhjd->nhij', query_heads, key_heads, precision=highest) * within
    attended = jnp.einsum('nhpd,nhde->nhpe', query_heads * growth[..., None], start_state, precision=highest) + jnp.einsum('nhij,nhje->nhie', scores, corrected, precision=highest)
    states = growth[..., None, None] * start_state[:, :, None] + jnp.einsum('nhtj,nhjd,nhje->nhtde', within, key_heads, corrected, precision=highest)
    return (attended, states)

def combine_heads(query_logits, key_logits, value_logits, beta_logits, decay_logits, head_decay_rate, token_extra_decay, accepted, prior_step_states, output_norm_gain):
    seq_count, proposal_len, head_count = beta_logits.shape
    head_size = query_logits.shape[-1] // head_count

    def by_heads(values):
        return jnp.transpose(values.reshape(seq_count, proposal_len, head_count, head_size), (0, 2, 1, 3))
    query_heads = unit_rows(by_heads(jax.nn.silu(query_logits))) * head_size ** (-0.5)
    key_heads = unit_rows(by_heads(jax.nn.silu(key_logits)))
    value_heads = by_heads(jax.nn.silu(value_logits))
    beta_gate = jnp.transpose(jax.nn.sigmoid(beta_logits), (0, 2, 1))
    decay_logarithm = jnp.transpose(-head_decay_rate[None, None, :] * jax.nn.softplus(decay_logits) + token_extra_decay, (0, 2, 1))
    chosen = jnp.arange(proposal_len, dtype=jnp.int32)[None, :] == (accepted - 1)[:, None]
    picked = lax.optimization_barrier(jnp.sum(jnp.where(chosen[:, :, None, None], prior_step_states, 0.0), axis=1))
    start_state = picked.reshape(seq_count, head_count, head_size, head_size)
    attended, states = delta_block(query_heads, key_heads, value_heads, beta_gate, decay_logarithm, start_state)
    inverse_rms = lax.rsqrt(lax.optimization_barrier(jnp.mean(attended * attended, axis=-1, keepdims=True)) + epsilon)
    normalized_rows = (attended * inverse_rms * output_norm_gain).astype(jnp.bfloat16)
    normalized_rows = jnp.transpose(normalized_rows, (0, 2, 1, 3)).reshape(seq_count, proposal_len, head_count * head_size)
    updated_states = jnp.transpose(states, (0, 2, 1, 3, 4)).reshape(seq_count, proposal_len, head_count, head_size * head_size)
    return (normalized_rows, updated_states)

def reference(tokens, input_norm_gain, query_projection, key_projection, value_projection, write_strength_weight, decay_projection, head_decay_rate, token_extra_decay, accepted, prior_step_states, output_norm_gain, output_projection):
    seq_total, proposal_len, feature_count = tokens.shape
    token_rows = tokens.reshape(seq_total * proposal_len, feature_count).astype(jnp.float32)
    inverse = lax.rsqrt(lax.optimization_barrier(jnp.sum(token_rows * token_rows, axis=1)) / feature_count + epsilon)[:, None]
    scaled = (token_rows * input_norm_gain[None, :]).astype(jnp.bfloat16)

    def apply_projection(weight):
        result = jnp.dot(scaled, weight, preferred_element_type=jnp.float32) * inverse
        return result.reshape(seq_total, proposal_len, weight.shape[1])
    block_count = seq_total // SEQ_DEV

    def divide_blocks(values):
        return values.reshape((block_count, SEQ_DEV) + values.shape[1:])

    def single_block(input_rows):
        query_logits, key_logits, value_logits, beta_logits, decay_logits, extra_decay_slice, accepted_slice, saved_slice = input_rows
        return combine_heads(query_logits, key_logits, value_logits, beta_logits, decay_logits, head_decay_rate, extra_decay_slice, accepted_slice, saved_slice, output_norm_gain)
    normalized_rows, updated_states = lax.map(single_block, (divide_blocks(apply_projection(query_projection)), divide_blocks(apply_projection(key_projection)), divide_blocks(apply_projection(value_projection)), divide_blocks(apply_projection(write_strength_weight)), divide_blocks(apply_projection(decay_projection)), divide_blocks(token_extra_decay), divide_blocks(accepted), divide_blocks(prior_step_states)))
    normed_rows = normalized_rows.reshape(seq_total * proposal_len, output_projection.shape[0])
    mixed = jnp.dot(normed_rows, output_projection, preferred_element_type=jnp.float32).astype(jnp.bfloat16)
    return (mixed.reshape(seq_total, proposal_len, feature_count), updated_states.reshape(prior_step_states.shape))
```

```python
import functools
import jax
import jax.numpy as jnp
from jax import lax
from jax.experimental import pallas as pl
from jax.experimental.pallas import tpu as pltpu
from jax.sharding import PartitionSpec as P

epsilon = 1e-06
MESH = pl.DeviceIdType.MESH
f32 = jnp.float32
bf16 = jnp.bfloat16
LANES = 128


def far_first(n):
    return sorted(range(1, n), key=lambda o: (abs(2 * o - n), o))


def near_first(n):
    return sorted(range(1, n), key=lambda o: (-abs(2 * o - n), o))


def silu(u):
    return u / (1.0 + jnp.exp(-u))


def kernel(
    n,
    ntp,
    head_size,
    tokens_hbm,
    gain_hbm,
    wq_hbm,
    wk_hbm,
    wv_hbm,
    wb_hbm,
    wd_hbm,
    rate_hbm,
    extra_hbm,
    accepted_hbm,
    prior_hbm,
    onorm_hbm,
    wo_hbm,
    mixed_ref,
    states_hbm,
    tokens_v,
    gain_v,
    w_v,
    wb_v,
    wd_v,
    rate_v,
    extra_v,
    accepted_s,
    prior_v,
    onorm_v,
    wo_v,
    x_v,
    part_v,
    aux_v,
    send_v,
    recv_v,
    recva_v,
    heads_v,
    gates_v,
    spread_v,
    expand_v,
    states_v,
    att_v,
    flat_v,
    normed_v,
    recvn_v,
    outp_v,
    recvp_v,
    load_sem,
    store_sem,
    rs_send,
    rs_recv,
    ag_send,
    ag_recv,
    tp_send,
    tp_recv,
):
    me = lax.axis_index("kv")
    my_tp = lax.axis_index("tp")
    group_seqs, steps, feature_dev = tokens_v.shape
    own_seqs, _, heads, state_len = prior_v.shape
    own_rows = own_seqs * steps
    model_width = n * feature_dev

    barrier = pltpu.get_barrier_semaphore()
    for o in far_first(n):
        pl.semaphore_signal(
            barrier, inc=1, device_id={"kv": lax.rem(me + o, n)}, device_id_type=MESH
        )
    for o in range(1, ntp):
        pl.semaphore_signal(
            barrier, inc=1, device_id={"tp": lax.rem(my_tp + o, ntp)}, device_id_type=MESH
        )

    loads = {}
    for index, (name, source, target) in enumerate((
        ("tokens", tokens_hbm, tokens_v),
        ("gain", gain_hbm, gain_v),
        ("wb", wb_hbm, wb_v),
        ("wd", wd_hbm, wd_v),
        ("q", wq_hbm, w_v.at[0]),
        ("k", wk_hbm, w_v.at[1]),
        ("v", wv_hbm, w_v.at[2]),
        ("prior", prior_hbm, prior_v),
        ("rate", rate_hbm, rate_v),
        ("extra", extra_hbm, extra_v),
        ("accepted", accepted_hbm, accepted_s),
        ("onorm", onorm_hbm, onorm_v),
        ("wo", wo_hbm, wo_v),
    )):
        loads[name] = pltpu.make_async_copy(source, target, load_sem.at[index])
        loads[name].start()

    loads["tokens"].wait()
    loads["gain"].wait()
    for s in range(group_seqs):
        x_v[s * steps:(s + 1) * steps, :] = tokens_v[s].astype(f32)
    x = x_v[...]
    squares = jnp.sum(x * x, axis=1, keepdims=True)
    scaled = (x * gain_v[...]).astype(bf16)

    contract_last = (((1,), (1,)), ((), ()))
    loads["wb"].wait()
    loads["wd"].wait()
    beta_part = lax.dot_general(scaled, wb_v[...], contract_last, preferred_element_type=f32)
    decay_part = lax.dot_general(scaled, wd_v[...], contract_last, preferred_element_type=f32)
    lane = lax.broadcasted_iota(jnp.int32, (x.shape[0], LANES), 1)
    aux_v[...] = jnp.where(lane == 2 * heads, squares, 0.0).reshape(aux_v.shape)
    aux_v[:, :, 0:heads] = beta_part.reshape(n, own_rows, heads)
    aux_v[:, :, heads:2 * heads] = decay_part.reshape(n, own_rows, heads)

    pl.semaphore_wait(barrier, n - 1 + ntp - 1)

    sends = []
    rs = {}

    def remote(source, target, send_sem, recv_sem, device):
        copy = pltpu.make_async_remote_copy(
            src_ref=source,
            dst_ref=target,
            send_sem=send_sem,
            recv_sem=recv_sem,
            device_id=device,
            device_id_type=MESH,
        )
        copy.start()
        sends.append(copy)
        return copy

    for o in far_first(n):
        target = lax.rem(me + o, n)
        rs[3, o] = remote(
            aux_v.at[target], recva_v.at[o - 1], rs_send.at[3, o - 1], rs_recv.at[3, o - 1],
            {"kv": target},
        )
    for piece, name in enumerate(("q", "k", "v")):
        loads[name].wait()
        part = jnp.dot(scaled, w_v[piece], preferred_element_type=f32)
        part = part.reshape(n, own_rows, part.shape[1])
        part_v[piece] = part
        send_v[piece] = part.astype(bf16)
        for o in far_first(n):
            target = lax.rem(me + o, n)
            rs[piece, o] = remote(
                send_v.at[piece, target], recv_v.at[piece, o - 1],
                rs_send.at[piece, o - 1], rs_recv.at[piece, o - 1], {"kv": target},
            )

    entry = lax.broadcasted_iota(jnp.int32, spread_v.shape, 0)
    column = lax.broadcasted_iota(jnp.int32, spread_v.shape, 1)
    first = lax.rem(entry, head_size) * head_size
    spread_v[...] = jnp.where(
        (column >= first) & (column < first + head_size), 1.0, 0.0
    ).astype(bf16)

    for name in ("rate", "extra", "accepted", "onorm", "prior"):
        loads[name].wait()

    aux = aux_v[me]
    for o in near_first(n):
        rs[3, o].wait_recv()
        aux = aux + recva_v[o - 1]
    inverse = lax.rsqrt(aux[:, 2 * heads:2 * heads + 1] / model_width + epsilon)
    pre = aux * inverse
    beta_pre = pre[:, 0:heads]
    decay_pre = pre[:, heads:2 * heads]
    softplus = jnp.maximum(decay_pre, 0.0) + jnp.log1p(jnp.exp(-jnp.abs(decay_pre)))
    extra = jnp.concatenate([extra_v[s] for s in range(own_seqs)], axis=0)
    gates_v[...] = jnp.zeros(gates_v.shape, f32)
    gates_v[:, 0:heads] = 1.0 / (1.0 + jnp.exp(-beta_pre))
    gates_v[:, heads:2 * heads] = jnp.exp(-rate_v[...] * softplus + extra)
    gates = gates_v[...].T

    def summed(piece):
        total = part_v[piece, me]
        for o in near_first(n):
            rs[piece, o].wait_recv()
            total = total + recv_v[piece, o - 1].astype(f32)
        value = silu(total * inverse)
        for h in range(heads):
            heads_v[piece, :, h, :] = value[:, h * head_size:(h + 1) * head_size]
        return heads_v[piece]

    def unit(value):
        return value * lax.rsqrt(jnp.sum(value * value, axis=-1, keepdims=True) + epsilon)

    tall = own_rows * heads
    for piece, scale in ((0, head_size ** -0.5), (1, 1.0)):
        value = (unit(summed(piece)) * scale).reshape(tall, head_size)
        high = value.astype(bf16)
        low = (value - high.astype(f32)).astype(bf16)
        both = jnp.concatenate([high.astype(f32), low.astype(f32)], axis=1).astype(bf16)
        expand_v[piece] = jnp.dot(both, spread_v[...], preferred_element_type=f32)
    value_heads = summed(2)

    def fold(product):
        width = product.shape[1]
        while width > LANES:
            width //= 2
            product = product[:, :width] + product[:, width:]
        return product + pltpu.roll(product, head_size, 1)

    stores = []
    for s in range(own_seqs):
        state = prior_v[s, jnp.clip(accepted_s[s] - 1, 0, steps - 1)]
        for t in range(steps):
            row = s * steps + t
            block = pl.ds(row * heads, heads)
            key_wide = expand_v[1, block, :]
            beta = gates[0:heads, row:row + 1]
            decay = gates[heads:2 * heads, row:row + 1]
            value = value_heads[row]
            value = jnp.concatenate([value] * (LANES // head_size), axis=1)
            write = beta * (value - decay * fold(key_wide * state))
            write = jnp.concatenate([write] * (state_len // LANES), axis=1)
            state = decay * state + key_wide * write
            states_v[s, t] = state
            copy = pltpu.make_async_copy(
                states_v.at[s, t], states_hbm.at[s, t], store_sem.at[row]
            )
            copy.start()
            stores.append(copy)
            attended = fold(expand_v[0, block, :] * state)
            att_v[row] = attended[:, 0:head_size]

    attended = att_v[...]
    mean = jnp.sum(attended * attended, axis=-1, keepdims=True) / head_size
    att_v[...] = attended * lax.rsqrt(mean + epsilon) * onorm_v[...].reshape(1, 1, head_size)
    for h in range(heads):
        flat_v[:, h * head_size:(h + 1) * head_size] = att_v[:, h, :]
    normed = flat_v[...].astype(bf16)
    normed_v[...] = normed

    gather = {}
    for o in far_first(n):
        gather[o] = remote(
            normed_v, recvn_v.at[o - 1], ag_send.at[o - 1], ag_recv.at[o - 1],
            {"kv": lax.rem(me + o, n)},
        )
    loads["wo"].wait()
    exchange = {}

    def project(o, rows):
        outp_v[o] = jnp.dot(rows, wo_v[...], preferred_element_type=f32).astype(bf16)
        for p in range(1, ntp):
            exchange[o, p] = remote(
                outp_v.at[o], recvp_v.at[p - 1, o], tp_send.at[p - 1, o], tp_recv.at[p - 1, o],
                {"tp": lax.rem(my_tp + p, ntp)},
            )

    order = [0] + near_first(n)
    project(0, normed)
    for o in near_first(n):
        gather[o].wait_recv()
        project(o, recvn_v[o - 1])
    for o in order:
        total = outp_v[o].astype(f32)
        for p in range(1, ntp):
            exchange[o, p].wait_recv()
            total = total + recvp_v[p - 1, o].astype(f32)
        mixed_ref[lax.rem(me - o + n, n)] = total.astype(bf16)

    for copy in sends:
        copy.wait_send()
    for copy in stores:
        copy.wait()


def per_device(n, ntp, *args):
    (
        tokens, input_norm_gain, query_projection, key_projection, value_projection,
        write_strength_weight, decay_projection, head_decay_rate, token_extra_decay,
        accepted, prior_step_states, output_norm_gain, output_projection,
    ) = args
    group_seqs, steps, feature_dev = tokens.shape
    own_seqs, _, heads, state_len = prior_step_states.shape
    own_rows = own_seqs * steps
    head_size = output_norm_gain.shape[0]
    inner = query_projection.shape[1]
    out_dev = output_projection.shape[1]
    rows = group_seqs * steps
    any_spec = pl.BlockSpec(memory_space=pl.ANY)
    dma = pltpu.SemaphoreType.DMA
    mixed, states = pl.pallas_call(
        functools.partial(kernel, n, ntp, head_size),
        out_shape=(
            jax.ShapeDtypeStruct((n, own_rows, out_dev), bf16),
            jax.ShapeDtypeStruct(prior_step_states.shape, f32),
        ),
        in_specs=[any_spec] * 13,
        out_specs=(pl.BlockSpec(memory_space=pltpu.VMEM), any_spec),
        scratch_shapes=[
            pltpu.VMEM(tokens.shape, bf16),
            pltpu.VMEM((1, feature_dev), f32),
            pltpu.VMEM((3, feature_dev, inner), bf16),
            pltpu.VMEM((heads, feature_dev), bf16),
            pltpu.VMEM((heads, feature_dev), bf16),
            pltpu.VMEM((1, heads), f32),
            pltpu.VMEM(token_extra_decay.shape, f32),
            pltpu.SMEM(accepted.shape, jnp.int32),
            pltpu.VMEM(prior_step_states.shape, f32),
            pltpu.VMEM((1, head_size), f32),
            pltpu.VMEM((inner, out_dev), bf16),
            pltpu.VMEM((rows, feature_dev), f32),
            pltpu.VMEM((3, n, own_rows, inner), f32),
            pltpu.VMEM((n, own_rows, LANES), f32),
            pltpu.VMEM((3, n, own_rows, inner), bf16),
            pltpu.VMEM((3, n - 1, own_rows, inner), bf16),
            pltpu.VMEM((n - 1, own_rows, LANES), f32),
            pltpu.VMEM((3, own_rows, heads, head_size), f32),
            pltpu.VMEM((own_rows, LANES), f32),
            pltpu.VMEM((2 * head_size, state_len), bf16),
            pltpu.VMEM((2, own_rows * heads, state_len), f32),
            pltpu.VMEM(prior_step_states.shape, f32),
            pltpu.VMEM((own_rows, heads, head_size), f32),
            pltpu.VMEM((own_rows, inner), f32),
            pltpu.VMEM((own_rows, inner), bf16),
            pltpu.VMEM((n - 1, own_rows, inner), bf16),
            pltpu.VMEM((n, own_rows, out_dev), bf16),
            pltpu.VMEM((ntp - 1, n, own_rows, out_dev), bf16),
            dma((13,)),
            dma((own_rows,)),
            dma((4, n - 1)),
            dma((4, n - 1)),
            dma((n - 1,)),
            dma((n - 1,)),
            dma((ntp - 1, n)),
            dma((ntp - 1, n)),
        ],
        compiler_params=pltpu.CompilerParams(collective_id=0, has_side_effects=True),
    )(
        tokens, input_norm_gain.reshape(1, feature_dev), query_projection, key_projection,
        value_projection, write_strength_weight.T, decay_projection.T,
        head_decay_rate.reshape(1, heads), token_extra_decay, accepted, prior_step_states,
        output_norm_gain.reshape(1, head_size), output_projection,
    )
    return mixed.reshape(group_seqs, steps, out_dev), states


def solution(mesh):
    in_specs = (
        P("dp", None, "kv"),
        P("kv"),
        P("kv", "tp"),
        P("kv", "tp"),
        P("kv", "tp"),
        P("kv", "tp"),
        P("kv", "tp"),
        P("tp"),
        P(("dp", "kv"), None, "tp"),
        P(("dp", "kv")),
        P(("dp", "kv"), None, "tp", None),
        P(),
        P("tp", "kv"),
    )
    out_specs = (P("dp", None, "kv"), P(("dp", "kv"), None, "tp", None))
    body = functools.partial(per_device, mesh.shape["kv"], mesh.shape["tp"])
    return jax.shard_map(
        body, mesh=mesh, in_specs=in_specs, out_specs=out_specs, check_vma=False
    )
```

```python
import functools
import jax
import jax.numpy as jnp
from jax import lax
from jax.experimental import pallas as pl
from jax.experimental.pallas import tpu as pltpu
from jax.sharding import PartitionSpec as P

epsilon = 1e-06
MESH = pl.DeviceIdType.MESH
f32 = jnp.float32
bf16 = jnp.bfloat16
LANES = 128
VMEM_LIMIT = 32 * 2 ** 20


def far_first(n):
    return sorted(range(1, n), key=lambda o: (abs(2 * o - n), o))


def near_first(n):
    return sorted(range(1, n), key=lambda o: (-abs(2 * o - n), o))


def silu(u):
    return u / (1.0 + jnp.exp(-u))


def kernel(
    n,
    ntp,
    head_size,
    tokens_hbm,
    gain_hbm,
    wq_hbm,
    wk_hbm,
    wv_hbm,
    wb_hbm,
    wd_hbm,
    rate_hbm,
    extra_hbm,
    accepted_hbm,
    prior_hbm,
    onorm_hbm,
    wo_hbm,
    mixed_ref,
    states_v,
    tokens_v,
    gain_v,
    w_v,
    wb_v,
    wd_v,
    rate_v,
    extra_v,
    accepted_s,
    prior_v,
    onorm_v,
    wo_v,
    x_v,
    part_v,
    aux_v,
    send_v,
    recv_v,
    recva_v,
    heads_v,
    gates_v,
    spread_v,
    expand_v,
    att_v,
    flat_v,
    normed_v,
    recvn_v,
    outp_v,
    recvp_v,
    load_sem,
    rs_send,
    rs_recv,
    ag_send,
    ag_recv,
    tp_send,
    tp_recv,
):
    me = lax.axis_index("kv")
    my_tp = lax.axis_index("tp")
    group_seqs, steps, feature_dev = tokens_v.shape
    own_seqs, _, heads, state_len = prior_v.shape
    own_rows = own_seqs * steps
    model_width = n * feature_dev

    barrier = pltpu.get_barrier_semaphore()
    for o in far_first(n):
        pl.semaphore_signal(
            barrier, inc=1, device_id={"kv": lax.rem(me + o, n)}, device_id_type=MESH
        )
    for o in range(1, ntp):
        pl.semaphore_signal(
            barrier, inc=1, device_id={"tp": lax.rem(my_tp + o, ntp)}, device_id_type=MESH
        )

    loads = {}
    for index, (name, source, target) in enumerate((
        ("tokens", tokens_hbm, tokens_v),
        ("gain", gain_hbm, gain_v),
        ("wb", wb_hbm, wb_v),
        ("wd", wd_hbm, wd_v),
        ("q", wq_hbm, w_v.at[0]),
        ("k", wk_hbm, w_v.at[1]),
        ("v", wv_hbm, w_v.at[2]),
        ("prior", prior_hbm, prior_v),
        ("rate", rate_hbm, rate_v),
        ("extra", extra_hbm, extra_v),
        ("accepted", accepted_hbm, accepted_s),
        ("onorm", onorm_hbm, onorm_v),
        ("wo", wo_hbm, wo_v),
    )):
        loads[name] = pltpu.make_async_copy(source, target, load_sem.at[index])
        loads[name].start()

    loads["tokens"].wait()
    loads["gain"].wait()
    for s in range(group_seqs):
        x_v[s * steps:(s + 1) * steps, :] = tokens_v[s].astype(f32)
    x = x_v[...]
    squares = jnp.sum(x * x, axis=1, keepdims=True)
    scaled = (x * gain_v[...]).astype(bf16)

    contract_last = (((1,), (1,)), ((), ()))
    loads["wb"].wait()
    loads["wd"].wait()
    beta_part = lax.dot_general(scaled, wb_v[...], contract_last, preferred_element_type=f32)
    decay_part = lax.dot_general(scaled, wd_v[...], contract_last, preferred_element_type=f32)
    lane = lax.broadcasted_iota(jnp.int32, (x.shape[0], LANES), 1)
    aux_v[...] = jnp.where(lane == 2 * heads, squares, 0.0).reshape(aux_v.shape)
    aux_v[:, :, 0:heads] = beta_part.reshape(n, own_rows, heads)
    aux_v[:, :, heads:2 * heads] = decay_part.reshape(n, own_rows, heads)

    pl.semaphore_wait(barrier, n - 1 + ntp - 1)

    sends = []
    rs = {}

    def remote(source, target, send_sem, recv_sem, device):
        copy = pltpu.make_async_remote_copy(
            src_ref=source,
            dst_ref=target,
            send_sem=send_sem,
            recv_sem=recv_sem,
            device_id=device,
            device_id_type=MESH,
        )
        copy.start()
        sends.append(copy)
        return copy

    for o in far_first(n):
        target = lax.rem(me + o, n)
        rs[3, o] = remote(
            aux_v.at[target], recva_v.at[o - 1], rs_send.at[3, o - 1], rs_recv.at[3, o - 1],
            {"kv": target},
        )
    for piece, name in enumerate(("q", "k", "v")):
        loads[name].wait()
        part = jnp.dot(scaled, w_v[piece], preferred_element_type=f32)
        part = part.reshape(n, own_rows, part.shape[1])
        part_v[piece] = part
        send_v[piece] = part.astype(bf16)
        for o in far_first(n):
            target = lax.rem(me + o, n)
            rs[piece, o] = remote(
                send_v.at[piece, target], recv_v.at[piece, o - 1],
                rs_send.at[piece, o - 1], rs_recv.at[piece, o - 1], {"kv": target},
            )

    entry = lax.broadcasted_iota(jnp.int32, spread_v.shape, 0)
    column = lax.broadcasted_iota(jnp.int32, spread_v.shape, 1)
    first = jnp.where(entry < head_size, entry, entry - head_size) * head_size
    spread_v[...] = jnp.where(
        (column >= first) & (column < first + head_size), 1.0, 0.0
    ).astype(bf16)

    for name in ("rate", "extra", "accepted", "onorm", "prior"):
        loads[name].wait()

    aux = aux_v[me]
    for o in near_first(n):
        rs[3, o].wait_recv()
        aux = aux + recva_v[o - 1]
    inverse = lax.rsqrt(aux[:, 2 * heads:2 * heads + 1] / model_width + epsilon)
    pre = aux * inverse
    beta_pre = pre[:, 0:heads]
    decay_pre = pre[:, heads:2 * heads]
    softplus = jnp.maximum(decay_pre, 0.0) + jnp.log1p(jnp.exp(-jnp.abs(decay_pre)))
    extra = jnp.concatenate([extra_v[s] for s in range(own_seqs)], axis=0)
    gates_v[...] = jnp.zeros(gates_v.shape, f32)
    gates_v[:, 0:heads] = 1.0 / (1.0 + jnp.exp(-beta_pre))
    gates_v[:, heads:2 * heads] = jnp.exp(-rate_v[...] * softplus + extra)
    gates = gates_v[...].T

    def summed(piece):
        total = part_v[piece, me]
        for o in near_first(n):
            rs[piece, o].wait_recv()
            total = total + recv_v[piece, o - 1].astype(f32)
        value = silu(total * inverse)
        for h in range(heads):
            heads_v[piece, :, h, :] = value[:, h * head_size:(h + 1) * head_size]
        return heads_v[piece]

    def unit(value):
        return value * lax.rsqrt(jnp.sum(value * value, axis=-1, keepdims=True) + epsilon)

    tall = own_rows * heads
    for piece, scale in ((0, head_size ** -0.5), (1, 1.0)):
        value = (unit(summed(piece)) * scale).reshape(tall, head_size)
        high = value.astype(bf16)
        low = (value - high.astype(f32)).astype(bf16)
        both = jnp.concatenate([high.astype(f32), low.astype(f32)], axis=1).astype(bf16)
        expand_v[piece] = jnp.dot(both, spread_v[...], preferred_element_type=f32)
    value_heads = summed(2)

    def fold(product):
        width = product.shape[1]
        while width > LANES:
            width //= 2
            product = product[:, :width] + product[:, width:]
        return product + pltpu.roll(product, head_size, 1)

    for s in range(own_seqs):
        state = prior_v[s, jnp.clip(accepted_s[s] - 1, 0, steps - 1)]
        for t in range(steps):
            row = s * steps + t
            block = pl.ds(row * heads, heads)
            key_wide = expand_v[1, block, :]
            beta = gates[0:heads, row:row + 1]
            decay = gates[heads:2 * heads, row:row + 1]
            value = value_heads[row]
            value = jnp.concatenate([value] * (LANES // head_size), axis=1)
            write = beta * (value - decay * fold(key_wide * state))
            write = jnp.concatenate([write] * (state_len // LANES), axis=1)
            state = decay * state + key_wide * write
            states_v[s, t] = state
            attended = fold(expand_v[0, block, :] * state)
            att_v[row] = attended[:, 0:head_size]

    attended = att_v[...]
    mean = jnp.sum(attended * attended, axis=-1, keepdims=True) / head_size
    att_v[...] = attended * lax.rsqrt(mean + epsilon) * onorm_v[...].reshape(1, 1, head_size)
    for h in range(heads):
        flat_v[:, h * head_size:(h + 1) * head_size] = att_v[:, h, :]
    normed = flat_v[...].astype(bf16)
    normed_v[...] = normed

    gather = {}
    for o in far_first(n):
        gather[o] = remote(
            normed_v, recvn_v.at[o - 1], ag_send.at[o - 1], ag_recv.at[o - 1],
            {"kv": lax.rem(me + o, n)},
        )
    loads["wo"].wait()
    exchange = {}

    def project(o, rows):
        outp_v[o] = jnp.dot(rows, wo_v[...], preferred_element_type=f32).astype(bf16)
        for p in range(1, ntp):
            exchange[o, p] = remote(
                outp_v.at[o], recvp_v.at[p - 1, o], tp_send.at[p - 1, o], tp_recv.at[p - 1, o],
                {"tp": lax.rem(my_tp + p, ntp)},
            )

    order = [0] + near_first(n)
    project(0, normed)
    for o in near_first(n):
        gather[o].wait_recv()
        project(o, recvn_v[o - 1])
    for o in order:
        total = outp_v[o].astype(f32)
        for p in range(1, ntp):
            exchange[o, p].wait_recv()
            total = total + recvp_v[p - 1, o].astype(f32)
        source = lax.rem(me - o + n, n) * own_seqs
        for s in range(own_seqs):
            mixed_ref[source + s] = total[s * steps:(s + 1) * steps].astype(bf16)

    for copy in sends:
        copy.wait_send()


def finish(mixed_v, states_v, mixed_hbm, states_hbm, sem):
    copies = (
        pltpu.make_async_copy(states_v, states_hbm, sem.at[0]),
        pltpu.make_async_copy(mixed_v, mixed_hbm, sem.at[1]),
    )
    for copy in copies:
        copy.start()
    for copy in copies:
        copy.wait()


def per_device(n, ntp, *args):
    (
        tokens, input_norm_gain, query_projection, key_projection, value_projection,
        write_strength_weight, decay_projection, head_decay_rate, token_extra_decay,
        accepted, prior_step_states, output_norm_gain, output_projection,
    ) = args
    group_seqs, steps, feature_dev = tokens.shape
    own_seqs, _, heads, state_len = prior_step_states.shape
    own_rows = own_seqs * steps
    head_size = output_norm_gain.shape[0]
    inner = query_projection.shape[1]
    out_dev = output_projection.shape[1]
    rows = group_seqs * steps
    any_spec = pl.BlockSpec(memory_space=pl.ANY)
    vmem_spec = pl.BlockSpec(memory_space=pltpu.VMEM)
    dma = pltpu.SemaphoreType.DMA

    def hbm(array):
        return pltpu.with_memory_space_constraint(array, pltpu.HBM)

    mixed, states = pl.pallas_call(
        functools.partial(kernel, n, ntp, head_size),
        out_shape=(
            pltpu.VMEM((group_seqs, steps, out_dev), bf16),
            pltpu.VMEM(prior_step_states.shape, f32),
        ),
        in_specs=[any_spec] * 13,
        out_specs=(vmem_spec, vmem_spec),
        scratch_shapes=[
            pltpu.VMEM(tokens.shape, bf16),
            pltpu.VMEM((1, feature_dev), f32),
            pltpu.VMEM((3, feature_dev, inner), bf16),
            pltpu.VMEM((heads, feature_dev), bf16),
            pltpu.VMEM((heads, feature_dev), bf16),
            pltpu.VMEM((1, heads), f32),
            pltpu.VMEM(token_extra_decay.shape, f32),
            pltpu.SMEM(accepted.shape, jnp.int32),
            pltpu.VMEM(prior_step_states.shape, f32),
            pltpu.VMEM((1, head_size), f32),
            pltpu.VMEM((inner, out_dev), bf16),
            pltpu.VMEM((rows, feature_dev), f32),
            pltpu.VMEM((3, n, own_rows, inner), f32),
            pltpu.VMEM((n, own_rows, LANES), f32),
            pltpu.VMEM((3, n, own_rows, inner), bf16),
            pltpu.VMEM((3, n - 1, own_rows, inner), bf16),
            pltpu.VMEM((n - 1, own_rows, LANES), f32),
            pltpu.VMEM((3, own_rows, heads, head_size), f32),
            pltpu.VMEM((own_rows, LANES), f32),
            pltpu.VMEM((2 * head_size, state_len), bf16),
            pltpu.VMEM((2, own_rows * heads, state_len), f32),
            pltpu.VMEM((own_rows, heads, head_size), f32),
            pltpu.VMEM((own_rows, inner), f32),
            pltpu.VMEM((own_rows, inner), bf16),
            pltpu.VMEM((n - 1, own_rows, inner), bf16),
            pltpu.VMEM((n, own_rows, out_dev), bf16),
            pltpu.VMEM((ntp - 1, n, own_rows, out_dev), bf16),
            dma((13,)),
            dma((4, n - 1)),
            dma((4, n - 1)),
            dma((n - 1,)),
            dma((n - 1,)),
            dma((ntp - 1, n)),
            dma((ntp - 1, n)),
        ],
        compiler_params=pltpu.CompilerParams(
            collective_id=0, has_side_effects=True, vmem_limit_bytes=VMEM_LIMIT
        ),
    )(*map(hbm, (
        tokens, input_norm_gain.reshape(1, feature_dev), query_projection, key_projection,
        value_projection, write_strength_weight.T, decay_projection.T,
        head_decay_rate.reshape(1, heads), token_extra_decay, accepted, prior_step_states,
        output_norm_gain.reshape(1, head_size), output_projection,
    )))
    return pl.pallas_call(
        finish,
        out_shape=(
            jax.ShapeDtypeStruct(mixed.shape, bf16),
            jax.ShapeDtypeStruct(states.shape, f32),
        ),
        in_specs=[vmem_spec, vmem_spec],
        out_specs=(any_spec, any_spec),
        scratch_shapes=[dma((2,))],
        compiler_params=pltpu.CompilerParams(vmem_limit_bytes=VMEM_LIMIT // 4),
    )(mixed, states)


def solution(mesh):
    in_specs = (
        P("dp", None, "kv"),
        P("kv"),
        P("kv", "tp"),
        P("kv", "tp"),
        P("kv", "tp"),
        P("kv", "tp"),
        P("kv", "tp"),
        P("tp"),
        P(("dp", "kv"), None, "tp"),
        P(("dp", "kv")),
        P(("dp", "kv"), None, "tp", None),
        P(),
        P("tp", "kv"),
    )
    out_specs = (P("dp", None, "kv"), P(("dp", "kv"), None, "tp", None))
    body = functools.partial(per_device, mesh.shape["kv"], mesh.shape["tp"])
    return jax.shard_map(
        body, mesh=mesh, in_specs=in_specs, out_specs=out_specs, check_vma=False
    )
```

```python
import functools
import jax
import jax.numpy as jnp
from jax import lax
from jax.experimental import pallas as pl
from jax.experimental.pallas import tpu as pltpu
from jax.sharding import PartitionSpec as P

epsilon = 1e-06
MESH = pl.DeviceIdType.MESH
f32 = jnp.float32
bf16 = jnp.bfloat16
LANES = 128
VMEM_LIMIT = 32 * 2 ** 20


def far_first(n):
    return sorted(range(1, n), key=lambda o: (abs(2 * o - n), o))


def near_first(n):
    return sorted(range(1, n), key=lambda o: (-abs(2 * o - n), o))


def silu(u):
    return u / (1.0 + jnp.exp(-u))


def kernel(
    n,
    ntp,
    head_size,
    tokens_hbm,
    gain_hbm,
    wq_hbm,
    wk_hbm,
    wv_hbm,
    wb_hbm,
    wd_hbm,
    rate_hbm,
    extra_hbm,
    accepted_hbm,
    prior_hbm,
    onorm_hbm,
    wo_hbm,
    mixed_ref,
    states_v,
    tokens_v,
    gain_v,
    w_v,
    wb_v,
    wd_v,
    rate_v,
    extra_v,
    accepted_s,
    prior_v,
    onorm_v,
    wo_v,
    x_v,
    part_v,
    aux_v,
    send_v,
    recv_v,
    recva_v,
    heads_v,
    gates_v,
    spread_v,
    expand_v,
    att_v,
    flat_v,
    normed_v,
    recvn_v,
    outp_v,
    recvp_v,
    load_sem,
    rs_send,
    rs_recv,
    ag_send,
    ag_recv,
    tp_send,
    tp_recv,
):
    me = lax.axis_index("kv")
    my_tp = lax.axis_index("tp")
    group_seqs, steps, feature_dev = tokens_v.shape
    own_seqs, _, heads, state_len = prior_v.shape
    own_rows = own_seqs * steps
    model_width = n * feature_dev

    barrier = pltpu.get_barrier_semaphore()
    for o in far_first(n):
        pl.semaphore_signal(
            barrier, inc=1, device_id={"kv": lax.rem(me + o, n)}, device_id_type=MESH
        )
    for o in range(1, ntp):
        pl.semaphore_signal(
            barrier, inc=1, device_id={"tp": lax.rem(my_tp + o, ntp)}, device_id_type=MESH
        )

    loads = {}
    for index, (name, source, target) in enumerate((
        ("tokens", tokens_hbm, tokens_v),
        ("gain", gain_hbm, gain_v),
        ("wb", wb_hbm, wb_v),
        ("wd", wd_hbm, wd_v),
        ("q", wq_hbm, w_v.at[0]),
        ("k", wk_hbm, w_v.at[1]),
        ("v", wv_hbm, w_v.at[2]),
        ("prior", prior_hbm, prior_v),
        ("rate", rate_hbm, rate_v),
        ("extra", extra_hbm, extra_v),
        ("accepted", accepted_hbm, accepted_s),
        ("onorm", onorm_hbm, onorm_v),
        ("wo", wo_hbm, wo_v),
    )):
        loads[name] = pltpu.make_async_copy(source, target, load_sem.at[index])
        loads[name].start()

    loads["tokens"].wait()
    loads["gain"].wait()
    for s in range(group_seqs):
        x_v[s * steps:(s + 1) * steps, :] = tokens_v[s].astype(f32)
    x = x_v[...]
    squares = jnp.sum(x * x, axis=1, keepdims=True)
    scaled = (x * gain_v[...]).astype(bf16)

    contract_last = (((1,), (1,)), ((), ()))
    loads["wb"].wait()
    loads["wd"].wait()
    beta_part = lax.dot_general(scaled, wb_v[...], contract_last, preferred_element_type=f32)
    decay_part = lax.dot_general(scaled, wd_v[...], contract_last, preferred_element_type=f32)
    lane = lax.broadcasted_iota(jnp.int32, (x.shape[0], LANES), 1)
    aux_v[...] = jnp.where(lane == 2 * heads, squares, 0.0).reshape(aux_v.shape)
    aux_v[:, :, 0:heads] = beta_part.reshape(n, own_rows, heads)
    aux_v[:, :, heads:2 * heads] = decay_part.reshape(n, own_rows, heads)

    def project_in(piece, name):
        loads[name].wait()
        part = jnp.dot(scaled, w_v[piece], preferred_element_type=f32)
        part = part.reshape(n, own_rows, part.shape[1])
        part_v[piece] = part
        send_v[piece] = part.astype(bf16)

    project_in(0, "q")
    pl.semaphore_wait(barrier, n - 1 + ntp - 1)

    sends = []
    rs = {}

    def remote(source, target, send_sem, recv_sem, device):
        copy = pltpu.make_async_remote_copy(
            src_ref=source,
            dst_ref=target,
            send_sem=send_sem,
            recv_sem=recv_sem,
            device_id=device,
            device_id_type=MESH,
        )
        copy.start()
        sends.append(copy)
        return copy

    for o in far_first(n):
        target = lax.rem(me + o, n)
        rs[3, o] = remote(
            aux_v.at[target], recva_v.at[o - 1], rs_send.at[3, o - 1], rs_recv.at[3, o - 1],
            {"kv": target},
        )
    for piece, name in enumerate(("q", "k", "v")):
        if piece > 0:
            project_in(piece, name)
        for o in far_first(n):
            target = lax.rem(me + o, n)
            rs[piece, o] = remote(
                send_v.at[piece, target], recv_v.at[piece, o - 1],
                rs_send.at[piece, o - 1], rs_recv.at[piece, o - 1], {"kv": target},
            )

    entry = lax.broadcasted_iota(jnp.int32, spread_v.shape, 0)
    column = lax.broadcasted_iota(jnp.int32, spread_v.shape, 1)
    first = jnp.where(entry < head_size, entry, entry - head_size) * head_size
    spread_v[...] = jnp.where(
        (column >= first) & (column < first + head_size), 1.0, 0.0
    ).astype(bf16)

    for name in ("rate", "extra", "accepted", "onorm", "prior"):
        loads[name].wait()

    aux = aux_v[me]
    for o in near_first(n):
        rs[3, o].wait_recv()
        aux = aux + recva_v[o - 1]
    inverse = lax.rsqrt(aux[:, 2 * heads:2 * heads + 1] / model_width + epsilon)
    pre = aux * inverse
    beta_pre = pre[:, 0:heads]
    decay_pre = pre[:, heads:2 * heads]
    softplus = jnp.maximum(decay_pre, 0.0) + jnp.log1p(jnp.exp(-jnp.abs(decay_pre)))
    extra = jnp.concatenate([extra_v[s] for s in range(own_seqs)], axis=0)
    gates_v[...] = jnp.zeros(gates_v.shape, f32)
    gates_v[:, 0:heads] = 1.0 / (1.0 + jnp.exp(-beta_pre))
    gates_v[:, heads:2 * heads] = jnp.exp(-rate_v[...] * softplus + extra)
    gates = gates_v[...].T

    def summed(piece):
        total = part_v[piece, me]
        for o in near_first(n):
            rs[piece, o].wait_recv()
            total = total + recv_v[piece, o - 1].astype(f32)
        value = silu(total * inverse)
        for h in range(heads):
            heads_v[piece, :, h, :] = value[:, h * head_size:(h + 1) * head_size]
        return heads_v[piece]

    def unit(value):
        return value * lax.rsqrt(jnp.sum(value * value, axis=-1, keepdims=True) + epsilon)

    tall = own_rows * heads
    for piece, scale in ((0, head_size ** -0.5), (1, 1.0)):
        value = (unit(summed(piece)) * scale).reshape(tall, head_size)
        high = value.astype(bf16)
        low = (value - high.astype(f32)).astype(bf16)
        both = jnp.concatenate([high.astype(f32), low.astype(f32)], axis=1).astype(bf16)
        expand_v[piece] = jnp.dot(both, spread_v[...], preferred_element_type=f32)
    value_heads = summed(2)

    def fold(product):
        width = product.shape[1]
        while width > LANES:
            width //= 2
            product = product[:, :width] + product[:, width:]
        return product + pltpu.roll(product, head_size, 1)

    current = [
        prior_v[s, jnp.clip(accepted_s[s] - 1, 0, steps - 1)] for s in range(own_seqs)
    ]
    for t in range(steps):
        for s in range(own_seqs):
            state = current[s]
            row = s * steps + t
            block = pl.ds(row * heads, heads)
            key_wide = expand_v[1, block, :]
            beta = gates[0:heads, row:row + 1]
            decay = gates[heads:2 * heads, row:row + 1]
            value = value_heads[row]
            value = jnp.concatenate([value] * (LANES // head_size), axis=1)
            write = beta * (value - decay * fold(key_wide * state))
            write = jnp.concatenate([write] * (state_len // LANES), axis=1)
            state = decay * state + key_wide * write
            states_v[s, t] = state
            current[s] = state
            attended = fold(expand_v[0, block, :] * state)
            att_v[row] = attended[:, 0:head_size]

    attended = att_v[...]
    mean = jnp.sum(attended * attended, axis=-1, keepdims=True) / head_size
    att_v[...] = attended * lax.rsqrt(mean + epsilon) * onorm_v[...].reshape(1, 1, head_size)
    for h in range(heads):
        flat_v[:, h * head_size:(h + 1) * head_size] = att_v[:, h, :]
    normed = flat_v[...].astype(bf16)
    normed_v[...] = normed

    gather = {}
    for o in far_first(n):
        gather[o] = remote(
            normed_v, recvn_v.at[o - 1], ag_send.at[o - 1], ag_recv.at[o - 1],
            {"kv": lax.rem(me + o, n)},
        )
    loads["wo"].wait()
    exchange = {}

    def project(o, rows):
        outp_v[o] = jnp.dot(rows, wo_v[...], preferred_element_type=f32).astype(bf16)
        for p in range(1, ntp):
            exchange[o, p] = remote(
                outp_v.at[o], recvp_v.at[p - 1, o], tp_send.at[p - 1, o], tp_recv.at[p - 1, o],
                {"tp": lax.rem(my_tp + p, ntp)},
            )

    order = [0] + near_first(n)
    project(0, normed)
    for o in near_first(n):
        gather[o].wait_recv()
        project(o, recvn_v[o - 1])
    for o in order:
        total = outp_v[o].astype(f32)
        for p in range(1, ntp):
            exchange[o, p].wait_recv()
            total = total + recvp_v[p - 1, o].astype(f32)
        source = lax.rem(me - o + n, n) * own_seqs
        for s in range(own_seqs):
            mixed_ref[source + s] = total[s * steps:(s + 1) * steps].astype(bf16)

    for copy in sends:
        copy.wait_send()


def finish(mixed_v, states_v, mixed_hbm, states_hbm, sem):
    own_seqs, steps = states_v.shape[:2]
    copies = [
        pltpu.make_async_copy(
            states_v.at[s, t], states_hbm.at[s, t], sem.at[1 + s * steps + t]
        )
        for s in range(own_seqs)
        for t in range(steps)
    ]
    copies.append(pltpu.make_async_copy(mixed_v, mixed_hbm, sem.at[0]))
    for copy in copies:
        copy.start()
    for copy in copies:
        copy.wait()


def per_device(n, ntp, *args):
    (
        tokens, input_norm_gain, query_projection, key_projection, value_projection,
        write_strength_weight, decay_projection, head_decay_rate, token_extra_decay,
        accepted, prior_step_states, output_norm_gain, output_projection,
    ) = args
    group_seqs, steps, feature_dev = tokens.shape
    own_seqs, _, heads, state_len = prior_step_states.shape
    own_rows = own_seqs * steps
    head_size = output_norm_gain.shape[0]
    inner = query_projection.shape[1]
    out_dev = output_projection.shape[1]
    rows = group_seqs * steps
    any_spec = pl.BlockSpec(memory_space=pl.ANY)
    vmem_spec = pl.BlockSpec(memory_space=pltpu.VMEM)
    dma = pltpu.SemaphoreType.DMA

    def hbm(array):
        return pltpu.with_memory_space_constraint(array, pltpu.HBM)

    mixed, states = pl.pallas_call(
        functools.partial(kernel, n, ntp, head_size),
        out_shape=(
            pltpu.VMEM((group_seqs, steps, out_dev), bf16),
            pltpu.VMEM(prior_step_states.shape, f32),
        ),
        in_specs=[any_spec] * 13,
        out_specs=(vmem_spec, vmem_spec),
        scratch_shapes=[
            pltpu.VMEM(tokens.shape, bf16),
            pltpu.VMEM((1, feature_dev), f32),
            pltpu.VMEM((3, feature_dev, inner), bf16),
            pltpu.VMEM((heads, feature_dev), bf16),
            pltpu.VMEM((heads, feature_dev), bf16),
            pltpu.VMEM((1, heads), f32),
            pltpu.VMEM(token_extra_decay.shape, f32),
            pltpu.SMEM(accepted.shape, jnp.int32),
            pltpu.VMEM(prior_step_states.shape, f32),
            pltpu.VMEM((1, head_size), f32),
            pltpu.VMEM((inner, out_dev), bf16),
            pltpu.VMEM((rows, feature_dev), f32),
            pltpu.VMEM((3, n, own_rows, inner), f32),
            pltpu.VMEM((n, own_rows, LANES), f32),
            pltpu.VMEM((3, n, own_rows, inner), bf16),
            pltpu.VMEM((3, n - 1, own_rows, inner), bf16),
            pltpu.VMEM((n - 1, own_rows, LANES), f32),
            pltpu.VMEM((3, own_rows, heads, head_size), f32),
            pltpu.VMEM((own_rows, LANES), f32),
            pltpu.VMEM((2 * head_size, state_len), bf16),
            pltpu.VMEM((2, own_rows * heads, state_len), f32),
            pltpu.VMEM((own_rows, heads, head_size), f32),
            pltpu.VMEM((own_rows, inner), f32),
            pltpu.VMEM((own_rows, inner), bf16),
            pltpu.VMEM((n - 1, own_rows, inner), bf16),
            pltpu.VMEM((n, own_rows, out_dev), bf16),
            pltpu.VMEM((ntp - 1, n, own_rows, out_dev), bf16),
            dma((13,)),
            dma((4, n - 1)),
            dma((4, n - 1)),
            dma((n - 1,)),
            dma((n - 1,)),
            dma((ntp - 1, n)),
            dma((ntp - 1, n)),
        ],
        compiler_params=pltpu.CompilerParams(
            collective_id=0, has_side_effects=True, vmem_limit_bytes=VMEM_LIMIT
        ),
    )(*map(hbm, (
        tokens, input_norm_gain.reshape(1, feature_dev), query_projection, key_projection,
        value_projection, write_strength_weight.T, decay_projection.T,
        head_decay_rate.reshape(1, heads), token_extra_decay, accepted, prior_step_states,
        output_norm_gain.reshape(1, head_size), output_projection,
    )))
    return pl.pallas_call(
        finish,
        out_shape=(
            jax.ShapeDtypeStruct(mixed.shape, bf16),
            jax.ShapeDtypeStruct(states.shape, f32),
        ),
        in_specs=[vmem_spec, vmem_spec],
        out_specs=(any_spec, any_spec),
        scratch_shapes=[dma((1 + own_rows,))],
        compiler_params=pltpu.CompilerParams(vmem_limit_bytes=VMEM_LIMIT // 4),
    )(mixed, states)


def solution(mesh):
    in_specs = (
        P("dp", None, "kv"),
        P("kv"),
        P("kv", "tp"),
        P("kv", "tp"),
        P("kv", "tp"),
        P("kv", "tp"),
        P("kv", "tp"),
        P("tp"),
        P(("dp", "kv"), None, "tp"),
        P(("dp", "kv")),
        P(("dp", "kv"), None, "tp", None),
        P(),
        P("tp", "kv"),
    )
    out_specs = (P("dp", None, "kv"), P(("dp", "kv"), None, "tp", None))
    body = functools.partial(per_device, mesh.shape["kv"], mesh.shape["tp"])
    return jax.shard_map(
        body, mesh=mesh, in_specs=in_specs, out_specs=out_specs, check_vma=False
    )
```

```python
import functools
import jax
import jax.numpy as jnp
from jax import lax
from jax.experimental import pallas as pl
from jax.experimental.pallas import tpu as pltpu
from jax.sharding import PartitionSpec as P

epsilon = 1e-06
MESH = pl.DeviceIdType.MESH
f32 = jnp.float32
bf16 = jnp.bfloat16
LANES = 128
VMEM_LIMIT = 32 * 2 ** 20


def far_first(n):
    return sorted(range(1, n), key=lambda o: (abs(2 * o - n), o))


def near_first(n):
    return sorted(range(1, n), key=lambda o: (-abs(2 * o - n), o))


def silu(u):
    return u / (1.0 + jnp.exp(-u))


def kernel(
    n,
    ntp,
    head_size,
    tokens_hbm,
    gain_hbm,
    wq_hbm,
    wk_hbm,
    wv_hbm,
    wb_hbm,
    wd_hbm,
    rate_hbm,
    extra_hbm,
    accepted_hbm,
    prior_hbm,
    onorm_hbm,
    wo_hbm,
    mixed_ref,
    states_v,
    tokens_v,
    gain_v,
    w_v,
    wb_v,
    wd_v,
    rate_v,
    extra_v,
    accepted_s,
    prior_v,
    onorm_v,
    wo_v,
    x_v,
    part_v,
    aux_v,
    send_v,
    recv_v,
    recva_v,
    heads_v,
    gates_v,
    spread_v,
    expand_v,
    att_v,
    flat_v,
    normed_v,
    recvn_v,
    outp_v,
    recvp_v,
    load_sem,
    rs_send,
    rs_recv,
    ag_send,
    ag_recv,
    tp_send,
    tp_recv,
):
    me = lax.axis_index("kv")
    my_tp = lax.axis_index("tp")
    group_seqs, steps, feature_dev = tokens_v.shape
    own_seqs, _, heads, state_len = prior_v.shape
    own_rows = own_seqs * steps
    model_width = n * feature_dev

    barrier = pltpu.get_barrier_semaphore()
    for o in far_first(n):
        pl.semaphore_signal(
            barrier, inc=1, device_id={"kv": lax.rem(me + o, n)}, device_id_type=MESH
        )
    for o in range(1, ntp):
        pl.semaphore_signal(
            barrier, inc=1, device_id={"tp": lax.rem(my_tp + o, ntp)}, device_id_type=MESH
        )

    loads = {}
    for index, (name, source, target) in enumerate((
        ("tokens", tokens_hbm, tokens_v),
        ("gain", gain_hbm, gain_v),
        ("wb", wb_hbm, wb_v),
        ("wd", wd_hbm, wd_v),
        ("q", wq_hbm, w_v.at[0]),
        ("k", wk_hbm, w_v.at[1]),
        ("v", wv_hbm, w_v.at[2]),
        ("prior", prior_hbm, prior_v),
        ("rate", rate_hbm, rate_v),
        ("extra", extra_hbm, extra_v),
        ("accepted", accepted_hbm, accepted_s),
        ("onorm", onorm_hbm, onorm_v),
        ("wo", wo_hbm, wo_v),
    )):
        loads[name] = pltpu.make_async_copy(source, target, load_sem.at[index])
        loads[name].start()

    loads["tokens"].wait()
    loads["gain"].wait()
    for s in range(group_seqs):
        x_v[s * steps:(s + 1) * steps, :] = tokens_v[s].astype(f32)
    x = x_v[...]
    squares = jnp.sum(x * x, axis=1, keepdims=True)
    scaled = (x * gain_v[...]).astype(bf16)

    contract_last = (((1,), (1,)), ((), ()))
    loads["wb"].wait()
    loads["wd"].wait()
    beta_part = lax.dot_general(scaled, wb_v[...], contract_last, preferred_element_type=f32)
    decay_part = lax.dot_general(scaled, wd_v[...], contract_last, preferred_element_type=f32)
    lane = lax.broadcasted_iota(jnp.int32, (x.shape[0], LANES), 1)
    aux_v[...] = jnp.where(lane == 2 * heads, squares, 0.0).reshape(aux_v.shape)
    aux_v[:, :, 0:heads] = beta_part.reshape(n, own_rows, heads)
    aux_v[:, :, heads:2 * heads] = decay_part.reshape(n, own_rows, heads)

    def project_in(piece, name):
        loads[name].wait()
        part = jnp.dot(scaled, w_v[piece], preferred_element_type=f32)
        part = part.reshape(n, own_rows, part.shape[1])
        part_v[piece] = part
        send_v[:, piece] = part.astype(bf16)

    project_in(0, "q")
    pl.semaphore_wait(barrier, n - 1 + ntp - 1)

    sends = []
    rs = {}

    def remote(source, target, send_sem, recv_sem, device):
        copy = pltpu.make_async_remote_copy(
            src_ref=source,
            dst_ref=target,
            send_sem=send_sem,
            recv_sem=recv_sem,
            device_id=device,
            device_id_type=MESH,
        )
        copy.start()
        sends.append(copy)
        return copy

    for o in far_first(n):
        target = lax.rem(me + o, n)
        rs[3, o] = remote(
            aux_v.at[target], recva_v.at[o - 1], rs_send.at[3, o - 1], rs_recv.at[3, o - 1],
            {"kv": target},
        )
    for piece, span in ((0, pl.ds(0, 1)), (1, pl.ds(1, 2))):
        if piece > 0:
            project_in(1, "k")
            project_in(2, "v")
        for o in far_first(n):
            target = lax.rem(me + o, n)
            rs[piece, o] = remote(
                send_v.at[target, span], recv_v.at[o - 1, span],
                rs_send.at[piece, o - 1], rs_recv.at[piece, o - 1], {"kv": target},
            )

    entry = lax.broadcasted_iota(jnp.int32, spread_v.shape, 0)
    column = lax.broadcasted_iota(jnp.int32, spread_v.shape, 1)
    first = jnp.where(entry < head_size, entry, entry - head_size) * head_size
    spread_v[...] = jnp.where(
        (column >= first) & (column < first + head_size), 1.0, 0.0
    ).astype(bf16)

    for name in ("rate", "extra", "accepted", "onorm", "prior"):
        loads[name].wait()

    aux = aux_v[me]
    for o in near_first(n):
        rs[3, o].wait_recv()
        aux = aux + recva_v[o - 1]
    inverse = lax.rsqrt(aux[:, 2 * heads:2 * heads + 1] / model_width + epsilon)
    pre = aux * inverse
    beta_pre = pre[:, 0:heads]
    decay_pre = pre[:, heads:2 * heads]
    softplus = jnp.maximum(decay_pre, 0.0) + jnp.log1p(jnp.exp(-jnp.abs(decay_pre)))
    extra = jnp.concatenate([extra_v[s] for s in range(own_seqs)], axis=0)
    gates_v[...] = jnp.zeros(gates_v.shape, f32)
    gates_v[:, 0:heads] = 1.0 / (1.0 + jnp.exp(-beta_pre))
    gates_v[:, heads:2 * heads] = jnp.exp(-rate_v[...] * softplus + extra)
    gates = gates_v[...].T

    def summed(piece):
        total = part_v[piece, me]
        for o in near_first(n):
            if piece < 2:
                rs[piece, o].wait_recv()
            total = total + recv_v[o - 1, piece].astype(f32)
        value = silu(total * inverse)
        for h in range(heads):
            heads_v[piece, :, h, :] = value[:, h * head_size:(h + 1) * head_size]
        return heads_v[piece]

    def unit(value):
        return value * lax.rsqrt(jnp.sum(value * value, axis=-1, keepdims=True) + epsilon)

    tall = own_rows * heads
    for piece, scale in ((0, head_size ** -0.5), (1, 1.0)):
        value = (unit(summed(piece)) * scale).reshape(tall, head_size)
        high = value.astype(bf16)
        low = (value - high.astype(f32)).astype(bf16)
        both = jnp.concatenate([high.astype(f32), low.astype(f32)], axis=1).astype(bf16)
        expand_v[piece] = jnp.dot(both, spread_v[...], preferred_element_type=f32)
    value_heads = summed(2)

    def fold(product):
        width = product.shape[1]
        while width > LANES:
            width //= 2
            product = product[:, :width] + product[:, width:]
        return product + pltpu.roll(product, head_size, 1)

    current = [
        prior_v[s, jnp.clip(accepted_s[s] - 1, 0, steps - 1)] for s in range(own_seqs)
    ]
    for t in range(steps):
        for s in range(own_seqs):
            state = current[s]
            row = s * steps + t
            block = pl.ds(row * heads, heads)
            key_wide = expand_v[1, block, :]
            beta = gates[0:heads, row:row + 1]
            decay = gates[heads:2 * heads, row:row + 1]
            value = value_heads[row]
            value = jnp.concatenate([value] * (LANES // head_size), axis=1)
            write = beta * (value - decay * fold(key_wide * state))
            write = jnp.concatenate([write] * (state_len // LANES), axis=1)
            state = decay * state + key_wide * write
            states_v[s, t] = state
            current[s] = state
            attended = fold(expand_v[0, block, :] * state)
            att_v[row] = attended[:, 0:head_size]

    attended = att_v[...]
    mean = jnp.sum(attended * attended, axis=-1, keepdims=True) / head_size
    att_v[...] = attended * lax.rsqrt(mean + epsilon) * onorm_v[...].reshape(1, 1, head_size)
    for h in range(heads):
        flat_v[:, h * head_size:(h + 1) * head_size] = att_v[:, h, :]
    normed = flat_v[...].astype(bf16)
    normed_v[...] = normed

    gather = {}
    for o in far_first(n):
        gather[o] = remote(
            normed_v, recvn_v.at[o - 1], ag_send.at[o - 1], ag_recv.at[o - 1],
            {"kv": lax.rem(me + o, n)},
        )
    loads["wo"].wait()
    exchange = {}

    def project(o, rows):
        outp_v[o] = jnp.dot(rows, wo_v[...], preferred_element_type=f32).astype(bf16)
        for p in range(1, ntp):
            exchange[o, p] = remote(
                outp_v.at[o], recvp_v.at[p - 1, o], tp_send.at[p - 1, o], tp_recv.at[p - 1, o],
                {"tp": lax.rem(my_tp + p, ntp)},
            )

    order = [0] + near_first(n)
    project(0, normed)
    for o in near_first(n):
        gather[o].wait_recv()
        project(o, recvn_v[o - 1])
    for o in order:
        total = outp_v[o].astype(f32)
        for p in range(1, ntp):
            exchange[o, p].wait_recv()
            total = total + recvp_v[p - 1, o].astype(f32)
        source = lax.rem(me - o + n, n) * own_seqs
        for s in range(own_seqs):
            mixed_ref[source + s] = total[s * steps:(s + 1) * steps].astype(bf16)

    for copy in sends:
        copy.wait_send()


def finish(mixed_v, states_v, mixed_hbm, states_hbm, sem):
    own_seqs, steps = states_v.shape[:2]
    copies = [
        pltpu.make_async_copy(
            states_v.at[s, t], states_hbm.at[s, t], sem.at[1 + s * steps + t]
        )
        for s in range(own_seqs)
        for t in range(steps)
    ]
    copies.append(pltpu.make_async_copy(mixed_v, mixed_hbm, sem.at[0]))
    for copy in copies:
        copy.start()
    for copy in copies:
        copy.wait()


def per_device(n, ntp, *args):
    (
        tokens, input_norm_gain, query_projection, key_projection, value_projection,
        write_strength_weight, decay_projection, head_decay_rate, token_extra_decay,
        accepted, prior_step_states, output_norm_gain, output_projection,
    ) = args
    group_seqs, steps, feature_dev = tokens.shape
    own_seqs, _, heads, state_len = prior_step_states.shape
    own_rows = own_seqs * steps
    head_size = output_norm_gain.shape[0]
    inner = query_projection.shape[1]
    out_dev = output_projection.shape[1]
    rows = group_seqs * steps
    any_spec = pl.BlockSpec(memory_space=pl.ANY)
    vmem_spec = pl.BlockSpec(memory_space=pltpu.VMEM)
    dma = pltpu.SemaphoreType.DMA

    def hbm(array):
        return pltpu.with_memory_space_constraint(array, pltpu.HBM)

    mixed, states = pl.pallas_call(
        functools.partial(kernel, n, ntp, head_size),
        out_shape=(
            pltpu.VMEM((group_seqs, steps, out_dev), bf16),
            pltpu.VMEM(prior_step_states.shape, f32),
        ),
        in_specs=[any_spec] * 13,
        out_specs=(vmem_spec, vmem_spec),
        scratch_shapes=[
            pltpu.VMEM(tokens.shape, bf16),
            pltpu.VMEM((1, feature_dev), f32),
            pltpu.VMEM((3, feature_dev, inner), bf16),
            pltpu.VMEM((heads, feature_dev), bf16),
            pltpu.VMEM((heads, feature_dev), bf16),
            pltpu.VMEM((1, heads), f32),
            pltpu.VMEM(token_extra_decay.shape, f32),
            pltpu.SMEM(accepted.shape, jnp.int32),
            pltpu.VMEM(prior_step_states.shape, f32),
            pltpu.VMEM((1, head_size), f32),
            pltpu.VMEM((inner, out_dev), bf16),
            pltpu.VMEM((rows, feature_dev), f32),
            pltpu.VMEM((3, n, own_rows, inner), f32),
            pltpu.VMEM((n, own_rows, LANES), f32),
            pltpu.VMEM((n, 3, own_rows, inner), bf16),
            pltpu.VMEM((n - 1, 3, own_rows, inner), bf16),
            pltpu.VMEM((n - 1, own_rows, LANES), f32),
            pltpu.VMEM((3, own_rows, heads, head_size), f32),
            pltpu.VMEM((own_rows, LANES), f32),
            pltpu.VMEM((2 * head_size, state_len), bf16),
            pltpu.VMEM((2, own_rows * heads, state_len), f32),
            pltpu.VMEM((own_rows, heads, head_size), f32),
            pltpu.VMEM((own_rows, inner), f32),
            pltpu.VMEM((own_rows, inner), bf16),
            pltpu.VMEM((n - 1, own_rows, inner), bf16),
            pltpu.VMEM((n, own_rows, out_dev), bf16),
            pltpu.VMEM((ntp - 1, n, own_rows, out_dev), bf16),
            dma((13,)),
            dma((4, n - 1)),
            dma((4, n - 1)),
            dma((n - 1,)),
            dma((n - 1,)),
            dma((ntp - 1, n)),
            dma((ntp - 1, n)),
        ],
        compiler_params=pltpu.CompilerParams(
            collective_id=0, has_side_effects=True, vmem_limit_bytes=VMEM_LIMIT
        ),
    )(*map(hbm, (
        tokens, input_norm_gain.reshape(1, feature_dev), query_projection, key_projection,
        value_projection, write_strength_weight.T, decay_projection.T,
        head_decay_rate.reshape(1, heads), token_extra_decay, accepted, prior_step_states,
        output_norm_gain.reshape(1, head_size), output_projection,
    )))
    return pl.pallas_call(
        finish,
        out_shape=(
            jax.ShapeDtypeStruct(mixed.shape, bf16),
            jax.ShapeDtypeStruct(states.shape, f32),
        ),
        in_specs=[vmem_spec, vmem_spec],
        out_specs=(any_spec, any_spec),
        scratch_shapes=[dma((1 + own_rows,))],
        compiler_params=pltpu.CompilerParams(vmem_limit_bytes=VMEM_LIMIT // 4),
    )(mixed, states)


def solution(mesh):
    in_specs = (
        P("dp", None, "kv"),
        P("kv"),
        P("kv", "tp"),
        P("kv", "tp"),
        P("kv", "tp"),
        P("kv", "tp"),
        P("kv", "tp"),
        P("tp"),
        P(("dp", "kv"), None, "tp"),
        P(("dp", "kv")),
        P(("dp", "kv"), None, "tp", None),
        P(),
        P("tp", "kv"),
    )
    out_specs = (P("dp", None, "kv"), P(("dp", "kv"), None, "tp", None))
    body = functools.partial(per_device, mesh.shape["kv"], mesh.shape["tp"])
    return jax.shard_map(
        body, mesh=mesh, in_specs=in_specs, out_specs=out_specs, check_vma=False
    )
```
